32 devices in a mesh: grp: 2 (over y), sp: 4 (over z), tp: 4 (over x, core).
Axes of the slice: x: 2, y: 2, z: 4, core: 2. Of those that a mesh axis runs over, the one named last changes fastest.
Arguments:
- recept: bfloat16 [4096, 2048], P(('grp', 'sp'), 'tp'), parts along dimension 0, may hold values from -6 to 6
- key_input: bfloat16 [4096, 2048], P(('grp', 'sp'), 'tp'), parts along dimension 0, may hold values from -6 to 6
- value_input: bfloat16 [4096, 2048], P(('grp', 'sp'), 'tp'), parts along dimension 0, may hold values from -6 to 6
- output_gate_input: bfloat16 [4096, 2048], P(('grp', 'sp'), 'tp'), parts along dimension 0, may hold values from -6 to 6
- decay_input_part: bfloat16 [4096, 2048], P(('grp', 'sp'), 'tp'), parts along dimension 0, may hold values from -4.8 to 4.8
- correction_rate_input: bfloat16 [4096, 2048], P(('grp', 'sp'), 'tp'), parts along dimension 0, may hold values from -4 to 4
- head_decay_offset: float32 [4096, 32], P(('grp', 'sp'), 'tp'), parts along dimension 0, may hold values from -2.1 to 0
- decay_fixed_bias: float32 [2048], P('tp'), may hold values from -11.5 to -2.8
- correction_rate_bias: float32 [2048], P('tp'), may hold values from -8.5 to 1
- head_norm_gain: float32 [2048], P('tp'), may hold values from 0.1 to 1.9
- self_term_weight: float32 [2048], P('tp'), may hold values from -2 to 2
- output_weight_matrix: bfloat16 [2048, 2048], P('tp'), may hold values from -0.125 to 0.125
- residual: bfloat16 [4096, 2048], P(('grp', 'sp', 'tp')), parts along dimension 0, may hold values from -6 to 6
- feedforward_norm_gain: float32 [2048], replicated, may hold values from 0.1 to 1.9
- routed_expert_index: int32 [4096, 2], P(('grp', 'sp', 'tp')), parts along dimension 0, may hold values from 0 to 3, all different within a row; in each aligned block of 128 rows (0 to 127, 128 to 255, ...) at most 96 rows name the same one
- routed_expert_weight: float32 [4096, 2], P(('grp', 'sp', 'tp')), parts along dimension 0, may hold values from 0.2 to 1
- gate_weight_experts: bfloat16 [4, 2048, 1024], P('sp', None, 'tp'), may hold values from -0.125 to 0.125
- up_weight_experts: bfloat16 [4, 2048, 1024], P('sp', None, 'tp'), may hold values from -0.125 to 0.125
- down_weight_experts: bfloat16 [4, 1024, 2048], P('sp', 'tp'), may hold values from -0.1875 to 0.1875
Outputs:
- output: bfloat16 [4096, 2048], P(('grp', 'sp', 'tp')), parts along dimension 0
The draws below stay inside these ranges and needn't reach their ends.
There are 2 independent parts, one for each index of `grp`. The reference program is written for one: setup_inputs(seed, part) draws one part's arguments, and reference() takes and returns one part's arrays. A program takes and returns all parts, laid end to end along the dimension named above; an argument that names none is the same for every part. Nothing has to cross between parts.
Inputs may be any that keep to these rules, and one draw needn't show every extreme that they name: `routed_expert_index`: in each aligned block of 128 rows (the rows of one device) no expert is named by more than 96 routes; the two experts of a row differ.
All inputs are finite; a program needn't handle non-finite values.
Results may differ from the reference program's by a relative error of at most 0.0058.
Values may be sent and summed in bfloat16 or wider, within the bound.
A program may use at most 128 MiB of HBM per device.

```python
import math
import jax
import jax.numpy as jnp
import numpy as np
from jax import lax

D = 2048
HEAD_COUNT = 32
HEAD_CHANNELS = 64
MODEL_WIDTH = 2048
FF = 1024
EXPERTS = 4
TOK_SP = 512
SEQUENCE_TOKENS = 2048
CAP = 96
N_SP = 4
N_TP = 4


def head_kinds(key):
    share = 5
    fast_heads = jax.random.randint(jax.random.fold_in(key, 11), (HEAD_COUNT,), 0, 10) < share
    return jnp.repeat(fast_heads, HEAD_CHANNELS)


def draw_decay_fixed_bias(key, part):
    fast_chan = head_kinds(key)
    uniform_draw = jax.random.uniform(jax.random.fold_in(key, 12), (MODEL_WIDTH,), jnp.float32)
    return jnp.where(fast_chan, -3.8 + uniform_draw, -11.5 + uniform_draw).astype(jnp.float32)


def draw_correction_rate_bias(key, part):
    fast_chan = head_kinds(key)
    uniform_draw = jax.random.uniform(jax.random.fold_in(key, 13), (MODEL_WIDTH,), jnp.float32)
    return jnp.where(fast_chan, -1.0 + 2.0 * uniform_draw, -8.5 + uniform_draw).astype(jnp.float32)


def draw_decay_input_part(key, part):
    noise = jnp.clip(jax.random.normal(jax.random.fold_in(key, 21), (SEQUENCE_TOKENS, MODEL_WIDTH), jnp.float32), -4.0, 4.0)
    shifts = jax.random.uniform(jax.random.fold_in(key, 22), (SEQUENCE_TOKENS // TOK_SP, 1, 1), jnp.float32, -0.8, 0.8)
    shaped = noise.reshape(SEQUENCE_TOKENS // TOK_SP, TOK_SP, MODEL_WIDTH) + shifts
    return shaped.reshape(SEQUENCE_TOKENS, MODEL_WIDTH).astype(jnp.bfloat16)


def draw_correction_rate_input(key, part):
    noise = jnp.clip(jax.random.normal(jax.random.fold_in(key, 31), (SEQUENCE_TOKENS, MODEL_WIDTH), jnp.float32), -4.0, 4.0)
    return noise.astype(jnp.bfloat16)


def draw_head_decay_offset(key, part):
    spots = jax.random.randint(jax.random.fold_in(key, 41), (3, HEAD_COUNT), 0, SEQUENCE_TOKENS)
    losses = jnp.log(jax.random.uniform(jax.random.fold_in(key, 42), (3, HEAD_COUNT), jnp.float32, 0.5, 0.8))
    places = jnp.arange(SEQUENCE_TOKENS, dtype=jnp.int32)[None, :, None]
    hits = places == spots[:, None, :]
    return jnp.sum(jnp.where(hits, losses[:, None, :], 0.0), axis=0).astype(jnp.float32)


def level_of(rng, dims, split, least, top_value):
    gain, own = 1.0, jax.random.fold_in(rng, 6)
    for dim, blocks in split:
        draws = jnp.exp(jax.random.uniform(jax.random.fold_in(own, dim), (blocks,), jnp.float32, least / len(split), top_value / len(split)))
        gain = gain * jnp.repeat(draws, dims[dim] // blocks).reshape([-1 if axis == dim else 1 for axis in range(len(dims))])
    return gain


def routed_block(rng, own, number, rows, amount, top, most, lean):
    sequence = jax.random.permutation(rng, amount)
    crowded, common = load_shares(amount, rows * top, most, lean, True), load_shares(amount, rows * top, most, lean, False)
    places = jnp.arange(amount)

    def named(sizes, turn):
        used = int((sizes > 0).sum())
        fixed = max(1, used // 4)
        moved = fixed + (places - fixed + turn * (used - fixed)) % max(1, amount - fixed)
        return jnp.zeros((amount,), jnp.int32).at[sequence[jnp.where(places < fixed, places, moved)]].set(jnp.asarray(sizes, jnp.int32))

    sizes = jnp.where(number % 4 == 0, named(crowded, number // 4), named(common, number - number // 4 - 1))
    mixed = jax.random.permutation(jax.random.fold_in(own, 3), amount)
    donor, receiver = mixed[0:amount // 2 * 2:2], mixed[1:amount // 2 * 2:2]
    slack = jnp.minimum(sizes[donor] - 1, most - sizes[receiver]) // 2
    slack = jnp.where((donor == sequence[0]) | (receiver == sequence[0]) | (sizes[receiver] == 0), 0, jnp.maximum(slack, 0))
    moved = jax.random.randint(jax.random.fold_in(own, 4), (amount // 2,), 0, 1 << 20) % (slack + 1)
    sizes = sizes.at[donor].add(-moved).at[receiver].add(moved)
    labels = jnp.searchsorted(jnp.cumsum(sizes), jnp.arange(rows * top), side="right").astype(jnp.int32)
    table = labels.reshape(top, rows).T
    table = table[jax.random.permutation(jax.random.fold_in(own, 1), rows)]
    turn = jax.random.randint(jax.random.fold_in(own, 2), (rows, 1), 0, top)
    return jnp.take_along_axis(table, (jnp.arange(top)[None, :] + turn) % top, axis=1)


def load_shares(count, total, limit, slope, full):
    portions = [(1 << 20) // math.isqrt(rank ** slope) + 1 for rank in range(1, count + 1)]
    largest = limit if full else min(limit, max(-(-total // count), total * portions[0] // sum(portions)))
    least = 1 if total - largest >= count - 1 else 0
    given, surplus = [largest] + [least] * (count - 1), total - largest - least * (count - 1)
    while surplus > 0:
        candidates = [i for i in range(1, count) if given[i] < largest] or [i for i in range(1, count) if given[i] < limit]
        whole, remaining = sum([portions[i] for i in candidates]), surplus
        for i in candidates:
            extra = min(limit - given[i], max(1, remaining * portions[i] // whole), surplus)
            given[i] = given[i] + extra
            surplus = surplus - extra
    return np.array(given)


def bell_draw(stream_key, dims, width, reach, shards=(), held_as=jnp.bfloat16):
    values = jax.random.normal(stream_key, dims, jnp.float32) * width
    if len(shards) > 0:
        values = level_of(stream_key, dims, shards, -0.22, 0.18) * values
    return jnp.clip(values, min=-reach, max=reach).astype(held_as)


def setup_inputs(seed: int = 0, part: int = 0) -> dict:
    streams_of = jax.random.split(jax.random.key(seed), 20)
    own_keys = jax.random.split(jax.random.fold_in(streams_of[19], part), 20)
    recept = bell_draw(own_keys[0], (SEQUENCE_TOKENS, MODEL_WIDTH), 1.0, 6.0, ((0, 4), (1, 4)))
    key_input = bell_draw(own_keys[1], (SEQUENCE_TOKENS, MODEL_WIDTH), 1.0, 6.0, ((0, 4), (1, 4)))
    value_input = bell_draw(own_keys[2], (SEQUENCE_TOKENS, MODEL_WIDTH), 1.0, 6.0, ((0, 4), (1, 4)))
    output_gate_input = bell_draw(own_keys[3], (SEQUENCE_TOKENS, MODEL_WIDTH), 1.0, 6.0, ((0, 4), (1, 4)))
    decay_input_part = draw_decay_input_part(jax.random.fold_in(jax.random.fold_in(streams_of[19], part), 71), part)
    correction_rate_input = draw_correction_rate_input(jax.random.fold_in(jax.random.fold_in(streams_of[19], part), 71), part)
    head_decay_offset = draw_head_decay_offset(jax.random.fold_in(jax.random.fold_in(streams_of[19], part), 71), part)
    decay_fixed_bias = draw_decay_fixed_bias(jax.random.fold_in(streams_of[19], 71), part)
    correction_rate_bias = draw_correction_rate_bias(jax.random.fold_in(streams_of[19], 71), part)
    head_norm_gain = jnp.clip(1.0 + 0.18 * jax.random.normal(streams_of[9], (MODEL_WIDTH,), jnp.float32), 0.1, 1.9)
    self_term_weight = bell_draw(streams_of[10], (MODEL_WIDTH,), 0.15, 2.0, ((0, 4),), jnp.float32)
    output_weight_matrix = bell_draw(streams_of[11], (MODEL_WIDTH, D), MODEL_WIDTH ** -0.5, 0.125, ((0, 4),))
    residual = bell_draw(own_keys[12], (SEQUENCE_TOKENS, D), 1.0, 6.0, ((0, 16),))
    feedforward_norm_gain = jnp.clip(1.0 + 0.18 * jax.random.normal(streams_of[13], (D,), jnp.float32), 0.1, 1.9)
    routed_expert_index_keys = jax.random.split(jax.random.fold_in(own_keys[14], 1), SEQUENCE_TOKENS // (TOK_SP // N_TP))
    routed_expert_index_turns = jax.random.permutation(jax.random.fold_in(own_keys[14], 3), SEQUENCE_TOKENS // (TOK_SP // N_TP))
    routed_expert_index = jax.vmap(lambda own, number: routed_block(jax.random.fold_in(own_keys[14], 2), own, number, TOK_SP // N_TP, EXPERTS, 2, CAP, 1))(routed_expert_index_keys, routed_expert_index_turns).reshape((SEQUENCE_TOKENS, 2))
    routed_expert_weight = jnp.clip(0.2 + 0.8 * jax.random.uniform(own_keys[15], (SEQUENCE_TOKENS, 2), jnp.float32) ** level_of(own_keys[15], (SEQUENCE_TOKENS, 2), ((0, 16),), -0.2, 0.2), 0.2, 1.0)
    gate_weight_experts = bell_draw(streams_of[16], (EXPERTS, D, FF), D ** -0.5, 0.125, ((0, 4), (2, 4)))
    up_weight_experts = bell_draw(streams_of[17], (EXPERTS, D, FF), D ** -0.5, 0.125, ((0, 4), (2, 4)))
    down_weight_experts = bell_draw(streams_of[18], (EXPERTS, FF, D), FF ** -0.5, 0.1875, ((0, 4), (1, 4)))
    return {"recept": recept, "key_input": key_input, "value_input": value_input, "output_gate_input": output_gate_input, "decay_input_part": decay_input_part, "correction_rate_input": correction_rate_input, "head_decay_offset": head_decay_offset, "decay_fixed_bias": decay_fixed_bias, "correction_rate_bias": correction_rate_bias, "head_norm_gain": head_norm_gain, "self_term_weight": self_term_weight, "output_weight_matrix": output_weight_matrix, "residual": residual, "feedforward_norm_gain": feedforward_norm_gain, "routed_expert_index": routed_expert_index, "routed_expert_weight": routed_expert_weight, "gate_weight_experts": gate_weight_experts, "up_weight_experts": up_weight_experts, "down_weight_experts": down_weight_experts}


PRECISE = lax.Precision.HIGHEST
GROUP_EPS = 0.00064
NORM_EPS = 1e-06

def recurrence(receptance_per_head, decay_per_head, key_per_head, value_per_head, remove_h, write_h):

    def advance(states, inputs):
        recept_t, decay_t, key_t, value_t, remove_t, write_t = inputs
        removed = jnp.einsum('hvk,hk->hv', states, remove_t, precision=PRECISE)
        states = states * decay_t[:, None, :] + removed[:, :, None] * write_t[:, None, :] + value_t[:, :, None] * key_t[:, None, :]
        return (states, jnp.einsum('hvk,hk->hv', states, recept_t, precision=PRECISE))
    initial = jnp.zeros((HEAD_COUNT, HEAD_CHANNELS, HEAD_CHANNELS), jnp.float32)
    _, readout = lax.scan(advance, initial, (receptance_per_head, decay_per_head, key_per_head, value_per_head, remove_h, write_h))
    return readout

def expert_rows(features, gate_mat, up_mat, down_mat):
    gated = jnp.dot(features, gate_mat, preferred_element_type=jnp.float32)
    upward = jnp.dot(features, up_mat, preferred_element_type=jnp.float32)
    hidden = (jax.nn.silu(gated) * upward).astype(jnp.bfloat16)
    blocks = jnp.einsum('rjf,jfd->rjd', hidden.reshape(features.shape[0], N_TP, FF // N_TP).astype(jnp.float32), down_mat.reshape(N_TP, FF // N_TP, D).astype(jnp.float32), precision=PRECISE)
    rounded = lax.optimization_barrier(blocks.astype(jnp.bfloat16)).astype(jnp.float32)
    return lax.optimization_barrier(jnp.sum(rounded, axis=1)).astype(jnp.bfloat16)

def reference(recept, key_input, value_input, output_gate_input, decay_input_part, correction_rate_input, head_decay_offset, decay_fixed_bias, correction_rate_bias, head_norm_gain, self_term_weight, output_weight_matrix, residual, feedforward_norm_gain, routed_expert_index, routed_expert_weight, gate_weight_experts, up_weight_experts, down_weight_experts):

    def split_into_heads(tensor):
        return tensor.astype(jnp.float32).reshape(SEQUENCE_TOKENS, HEAD_COUNT, HEAD_CHANNELS)
    receptance_per_head, key_per_head, value_per_head = (split_into_heads(recept), split_into_heads(key_input), split_into_heads(value_input))
    weight_logarithm = -jax.nn.softplus(-(decay_fixed_bias + decay_input_part.astype(jnp.float32))) - 0.5
    decay_per_head = jnp.exp(-jnp.exp(split_into_heads(weight_logarithm)) + head_decay_offset[:, :, None])
    rate_h = split_into_heads(jax.nn.sigmoid(correction_rate_bias + correction_rate_input.astype(jnp.float32)))
    unit_key = key_per_head * lax.rsqrt(lax.optimization_barrier(jnp.sum(key_per_head * key_per_head, axis=-1, keepdims=True)) + NORM_EPS)
    readout = recurrence(receptance_per_head, decay_per_head, key_per_head, value_per_head, -unit_key, unit_key * rate_h)
    center = lax.optimization_barrier(jnp.mean(readout, axis=-1, keepdims=True))
    spread = lax.optimization_barrier(jnp.mean(jnp.square(readout - center), axis=-1, keepdims=True))
    normalized_state = (readout - center) * lax.rsqrt(spread + GROUP_EPS) * head_norm_gain.reshape(HEAD_COUNT, HEAD_CHANNELS)
    self_term = lax.optimization_barrier(jnp.sum(receptance_per_head * key_per_head * self_term_weight.reshape(HEAD_COUNT, HEAD_CHANNELS), axis=-1, keepdims=True)) * value_per_head
    attention_result = ((normalized_state + self_term).reshape(SEQUENCE_TOKENS, MODEL_WIDTH) * output_gate_input.astype(jnp.float32)).astype(jnp.bfloat16)
    proj = jnp.dot(attention_result, output_weight_matrix, preferred_element_type=jnp.float32).astype(jnp.bfloat16)
    stream = residual.astype(jnp.float32) + lax.optimization_barrier(proj).astype(jnp.float32)
    ffn_in = (stream * lax.rsqrt(lax.optimization_barrier(jnp.mean(stream * stream, axis=-1, keepdims=True)) + NORM_EPS) * feedforward_norm_gain).astype(jnp.bfloat16)
    flat_ids = routed_expert_index.reshape(-1).astype(jnp.int32)
    flat_weights = routed_expert_weight.reshape(-1)
    top_count = routed_expert_index.shape[1]
    order = jnp.argsort(flat_ids, stable=True).astype(jnp.int32)
    counts = lax.optimization_barrier(jnp.sum((flat_ids[:, None] == jnp.arange(EXPERTS, dtype=jnp.int32)[None, :]).astype(jnp.int32), axis=0))
    starts = (jnp.cumsum(counts) - counts).astype(jnp.int32)
    room = N_SP * N_TP * CAP
    padded = jnp.concatenate([order, jnp.zeros((room,), jnp.int32)])

    def one_expert(accum, expert):
        entries = lax.dynamic_slice_in_dim(padded, starts[expert], room)
        live = jnp.arange(room, dtype=jnp.int32) < counts[expert]
        positions = (entries // top_count).astype(jnp.int32)
        result = expert_rows(ffn_in[positions], gate_weight_experts[expert], up_weight_experts[expert], down_weight_experts[expert])
        scales = jnp.where(live, flat_weights[entries], 0.0)
        return (accum.at[positions].add(result.astype(jnp.float32) * scales[:, None]), None)
    accum, _ = lax.scan(one_expert, jnp.zeros((SEQUENCE_TOKENS, D), jnp.float32), jnp.arange(EXPERTS, dtype=jnp.int32))
    return (stream + accum).astype(jnp.bfloat16)
```

```python
import functools

import jax
import jax.numpy as jnp
from jax import lax
from jax.experimental import pallas as pl
from jax.experimental.pallas import tpu as pltpu
from jax.sharding import PartitionSpec as P

SPAN = 64
SUB = 16
LANES = 256
GROUP_EPS = 0.00064
NORM_EPS = 1e-06
NN = (((1,), (0,)), ((), ()))
NT = (((1,), (1,)), ((), ()))
TN = (((0,), (0,)), ((), ()))


def halves(x):
    high = x.astype(jnp.bfloat16)
    return high, (x - high.astype(jnp.float32)).astype(jnp.bfloat16)


def product(left, right, dims):
    def dot(a, b):
        return lax.dot_general(a, b, dims, preferred_element_type=jnp.float32)

    return dot(left[0], right[0]) + (dot(left[1], right[0]) + dot(left[0], right[1]))


def block_mask(head_width):
    rows = lax.broadcasted_iota(jnp.int32, (LANES, LANES), 0) // head_width
    lanes = lax.broadcasted_iota(jnp.int32, (LANES, LANES), 1) // head_width
    return jnp.where(rows == lanes, 1.0, 0.0)


def spread_blocks(x, mask):
    copies = LANES // x.shape[0]
    return tuple(jnp.concatenate([part] * copies, axis=0) * mask for part in halves(x))


def head_sum(x, mask):
    high, low = halves(x)
    return lax.dot_general(
        high, mask, NN, preferred_element_type=jnp.float32
    ) + lax.dot_general(low, mask, NN, preferred_element_type=jnp.float32)


def chunk_kernel(
    head_width,
    recept_ref,
    key_ref,
    value_ref,
    decay_ref,
    rate_ref,
    offset_ref,
    decay_bias_ref,
    rate_bias_ref,
    map_ref,
    own_ref,
    transit_ref,
    added_ref,
):
    span = head_width
    wide_mask = block_mask(head_width)
    mask = wide_mask.astype(jnp.bfloat16)
    per_group = LANES // head_width
    times = lax.broadcasted_iota(jnp.int32, (span, LANES), 0)
    lanes = lax.broadcasted_iota(jnp.int32, (span, LANES), 1)
    earlier = lanes % head_width
    strict = times > earlier
    within = times >= earlier
    eye = jnp.where(times == earlier, 1.0, 0.0)
    same = (times // SUB) == (earlier // SUB)
    tri = jnp.where(
        lax.broadcasted_iota(jnp.int32, (span, span), 0)
        >= lax.broadcasted_iota(jnp.int32, (span, span), 1),
        1.0,
        0.0,
    ).astype(jnp.bfloat16)

    @pl.when(pl.program_id(0) == 0)
    def _():
        full_lanes = lax.broadcasted_iota(jnp.int32, transit_ref.shape, 1) % head_width
        full_rows = lax.broadcasted_iota(jnp.int32, transit_ref.shape, 0)
        transit_ref[...] = jnp.where(full_lanes == full_rows, 1.0, 0.0)
        added_ref[...] = jnp.zeros_like(added_ref)

    spread = functools.partial(spread_blocks, mask=mask)
    row_count, channel_width = recept_ref.shape
    cells = [
        (group, chunk)
        for chunk in range(row_count // span)
        for group in range(channel_width // LANES)
    ]

    def prepare(group, chunk):
        at = (slice(chunk * span, (chunk + 1) * span), slice(group * LANES, (group + 1) * LANES))
        cols = at[1]
        recept = recept_ref[at].astype(jnp.float32)
        key = key_ref[at].astype(jnp.float32)
        value = value_ref[at].astype(jnp.float32)
        offset = jnp.zeros((span, LANES), jnp.float32)
        for head in range(per_group):
            column = group * per_group + head
            offset = jnp.where(
                lanes // head_width == head, offset_ref[at[0], column : column + 1], offset
            )
        pre = decay_bias_ref[:, cols] + decay_ref[at].astype(jnp.float32)
        decay = offset - 0.6065306597126334 / (1.0 + jnp.exp(-pre))
        rate = 1.0 / (
            1.0 + jnp.exp(-(rate_bias_ref[:, cols] + rate_ref[at].astype(jnp.float32)))
        )
        unit = key * lax.rsqrt(head_sum(key * key, mask) + NORM_EPS)
        one, rest = halves(decay)
        third = (decay - one.astype(jnp.float32) - rest.astype(jnp.float32)).astype(jnp.bfloat16)
        cumul = sum(
            lax.dot_general(tri, part, NN, preferred_element_type=jnp.float32)
            for part in (third, rest, one)
        )
        middle = cumul[span // 2 : span // 2 + 1]
        last = cumul[span - 1 : span]
        center = cumul - middle
        shrink = jnp.exp(center)
        grow = jnp.exp(-center)
        remove = -unit * jnp.exp(center - decay)
        reads = recept * shrink
        write = unit * rate * grow
        keys = key * grow
        left = halves(jnp.concatenate([remove, reads], axis=0))
        by_write = product(left, spread(write), NT)
        by_key = product(left, spread(keys), NT)
        remove_write = jnp.where(strict, by_write[:span], 0.0)
        read_write = halves(jnp.where(within, by_write[span:], 0.0))
        key_rows = halves(
            jnp.concatenate(
                [jnp.where(strict, by_key[:span], 0.0), jnp.where(within, by_key[span:], 0.0)],
                axis=0,
            )
        )
        power = jnp.where(same, remove_write, 0.0)
        inverse = eye + power
        power = product(halves(power), spread(power), NN)
        reach = 2
        while reach < SUB:
            factor = spread(power)
            if reach * 2 < SUB:
                both = product(
                    halves(jnp.concatenate([inverse, power], axis=0)), factor, NN
                )
                inverse = inverse + both[:span]
                power = both[span:]
            else:
                inverse = inverse + product(halves(inverse), factor, NN)
            reach *= 2
        size = SUB
        while size < span:
            joint = (times // (2 * size) == earlier // (2 * size)) & (
                times // size != earlier // size
            )
            step = product(
                halves(inverse), spread(jnp.where(joint, remove_write, 0.0)), NN
            )
            inverse = inverse + product(halves(step), spread(inverse), NN)
            size *= 2
        inverse = halves(inverse)
        start = jnp.exp(middle)
        from_value = product(key_rows, spread(value), NN)
        inv_remove = product(inverse, spread(remove), NN) * start
        inv_value = product(inverse, spread(from_value[:span]), NN)
        read_map = reads * start + product(read_write, spread(inv_remove), NN)
        read_own = from_value[span:] + product(read_write, spread(inv_value), NN)
        tail = jnp.exp(last - middle)
        write_end = write * tail
        key_end = keys * tail
        transit = product(halves(inv_remove.T), halves(write_end), NN)
        transit = transit * wide_mask
        full = jnp.concatenate([jnp.exp(last)] * (LANES // 8), axis=0)
        full = jnp.concatenate([full] * 8, axis=0)
        diagonal = lax.broadcasted_iota(jnp.int32, (LANES, LANES), 0) == (
            lax.broadcasted_iota(jnp.int32, (LANES, LANES), 1)
        )
        transit = transit + jnp.where(diagonal, full, 0.0)
        added = product(
            halves(jnp.concatenate([inv_value, value], axis=0).T),
            halves(jnp.concatenate([write_end, key_end], axis=0)),
            NN,
        )
        added = added * wide_mask
        added = sum(added[h * head_width : (h + 1) * head_width] for h in range(per_group))
        return at, read_map, read_own, transit, added

    for group, chunk in cells:
        at, read_map, read_own, transit, added = prepare(group, chunk)
        cols = at[1]
        held_transit = transit_ref[:, cols]
        held_added = added_ref[:, cols]
        rows = halves(read_map)
        map_ref[at] = product(rows, spread(held_transit), NT)
        own_ref[at] = read_own + product(rows, spread(held_added), NT)
        moved = product(
            halves(jnp.concatenate([held_transit, held_added], axis=0)), halves(transit), NN
        )
        transit_ref[:, cols] = moved[:span]
        added_ref[:, cols] = moved[span:] + added


def advance_kernel(head_width, state_ref, transit_ref, added_ref, out_ref):
    mask = block_mask(head_width).astype(jnp.bfloat16)
    for group in range(state_ref.shape[1] // LANES):
        cols = slice(group * LANES, (group + 1) * LANES)
        out_ref[:, cols] = added_ref[:, cols] + product(
            halves(state_ref[:, cols]), spread_blocks(transit_ref[:, cols], mask), NN
        )


def finish_kernel(
    head_width,
    map_ref,
    own_ref,
    state_ref,
    recept_ref,
    key_ref,
    value_ref,
    gate_ref,
    gain_ref,
    self_ref,
    out_ref,
):
    mask = block_mask(head_width).astype(jnp.bfloat16)
    for group in range(map_ref.shape[1] // LANES):
        cols = slice(group * LANES, (group + 1) * LANES)
        read = own_ref[:, cols] + product(
            halves(map_ref[:, cols]), spread_blocks(state_ref[:, cols], mask), NT
        )
        off = read - head_sum(read, mask) * (1.0 / head_width)
        spread = head_sum(off * off, mask) * (1.0 / head_width)
        normed = off * lax.rsqrt(spread + GROUP_EPS) * gain_ref[:, cols]
        own = head_sum(
            recept_ref[:, cols].astype(jnp.float32)
            * key_ref[:, cols].astype(jnp.float32)
            * self_ref[:, cols],
            mask,
        ) * value_ref[:, cols].astype(jnp.float32)
        out_ref[:, cols] = ((normed + own) * gate_ref[:, cols].astype(jnp.float32)).astype(
            jnp.bfloat16
        )


def mixer(
    recept,
    key_input,
    value_input,
    output_gate_input,
    decay_input_part,
    correction_rate_input,
    head_decay_offset,
    decay_fixed_bias,
    correction_rate_bias,
    head_norm_gain,
    self_term_weight,
    axis_size,
):
    length, width = recept.shape
    heads = head_decay_offset.shape[1]
    head_width = width // heads
    rows = 2 * SPAN
    by_rows = pl.BlockSpec((rows, width), lambda i: (i, 0))
    fixed = pl.BlockSpec((1, width), lambda i: (0, 0))
    states = pl.BlockSpec((head_width, width), lambda i: (0, 0))
    wide = jax.ShapeDtypeStruct((length, width), jnp.float32)
    small = jax.ShapeDtypeStruct((head_width, width), jnp.float32)
    params = pltpu.CompilerParams(dimension_semantics=("arbitrary",))
    read_map, read_own, transit, added = pl.pallas_call(
        functools.partial(chunk_kernel, head_width),
        grid=(length // rows,),
        in_specs=[by_rows] * 5
        + [pl.BlockSpec((rows, heads), lambda i: (i, 0)), fixed, fixed],
        out_specs=[by_rows, by_rows, states, states],
        out_shape=[wide, wide, small, small],
        compiler_params=params,
        cost_estimate=pl.CostEstimate(
            flops=30_000_000_000, bytes_accessed=8 * length * width, transcendentals=0
        ),
        name="chunks",
    )(
        recept,
        key_input,
        value_input,
        decay_input_part,
        correction_rate_input,
        head_decay_offset,
        decay_fixed_bias[None],
        correction_rate_bias[None],
    )
    place = lax.axis_index("sp")
    state = jnp.zeros_like(added)
    for lap in range(axis_size - 1):
        sent = added
        if lap > 0:
            sent = pl.pallas_call(
                functools.partial(advance_kernel, head_width), out_shape=small, name="advance"
            )(state, transit, added)
        got = lax.ppermute(sent, "sp", [(i, i + 1) for i in range(axis_size - 1)])
        state = jnp.where(place == lap + 1, got, state)
    return pl.pallas_call(
        functools.partial(finish_kernel, head_width),
        grid=(length // rows,),
        in_specs=[by_rows, by_rows, states] + [by_rows] * 4 + [fixed, fixed],
        out_specs=by_rows,
        out_shape=jax.ShapeDtypeStruct((length, width), jnp.bfloat16),
        compiler_params=params,
        name="finish",
    )(
        read_map,
        read_own,
        state,
        recept,
        key_input,
        value_input,
        output_gate_input,
        head_norm_gain[None],
        self_term_weight[None],
    )


def local(
    recept,
    key_input,
    value_input,
    output_gate_input,
    decay_input_part,
    correction_rate_input,
    head_decay_offset,
    decay_fixed_bias,
    correction_rate_bias,
    head_norm_gain,
    self_term_weight,
    output_weight_matrix,
    residual,
    feedforward_norm_gain,
    routed_expert_index,
    routed_expert_weight,
    gate_weight_experts,
    up_weight_experts,
    down_weight_experts,
):
    gates = lax.all_gather(gate_weight_experts, "tp", axis=0)
    ups = lax.all_gather(up_weight_experts, "tp", axis=0)
    downs = lax.all_gather(down_weight_experts, "tp", axis=0)
    attention_result = mixer(
        recept,
        key_input,
        value_input,
        output_gate_input,
        decay_input_part,
        correction_rate_input,
        head_decay_offset,
        decay_fixed_bias,
        correction_rate_bias,
        head_norm_gain,
        self_term_weight,
        lax.axis_size("sp"),
    )
    proj = lax.psum_scatter(
        jnp.dot(
            attention_result, output_weight_matrix, preferred_element_type=jnp.float32
        ).astype(jnp.bfloat16),
        "tp",
        scatter_dimension=0,
        tiled=True,
    )
    stream = residual.astype(jnp.float32) + lax.optimization_barrier(proj).astype(jnp.float32)
    ffn_in = (
        stream
        * lax.rsqrt(jnp.mean(stream * stream, axis=-1, keepdims=True) + NORM_EPS)
        * feedforward_norm_gain
    ).astype(jnp.bfloat16)
    width = ffn_in.shape[1]
    local_experts = gate_weight_experts.shape[0]
    experts = local_experts * lax.axis_size("sp")
    ids = jnp.arange(experts, dtype=jnp.int32)
    shares = jnp.sum(
        jnp.where(
            routed_expert_index[:, :, None] == ids, routed_expert_weight[:, :, None], 0.0
        ),
        axis=1,
    )
    first = shares.astype(jnp.bfloat16)
    rest = shares - first.astype(jnp.float32)
    second = rest.astype(jnp.bfloat16)
    third = (rest - second.astype(jnp.float32)).astype(jnp.bfloat16)
    extra = jnp.concatenate([first, second, third], axis=1)
    extra = jnp.pad(extra, ((0, 0), (0, -extra.shape[1] % 128)))
    packed = lax.all_gather(
        jnp.concatenate([ffn_in, extra], axis=1), "sp", axis=0, tiled=True
    )
    features = packed[:, :width]
    tail = packed[:, width : width + 3 * experts].astype(jnp.float32)
    shares = tail[:, :experts] + tail[:, experts : 2 * experts] + tail[:, 2 * experts :]
    total = None
    for own in range(local_experts):
        expert = lax.axis_index("sp") * local_experts + own
        share = jnp.sum(jnp.where(ids[None, :] == expert, shares, 0.0), axis=1, keepdims=True)
        gated = jnp.einsum(
            "rd,jdf->jrf", features, gates[:, own], preferred_element_type=jnp.float32
        )
        upward = jnp.einsum(
            "rd,jdf->jrf", features, ups[:, own], preferred_element_type=jnp.float32
        )
        hidden = (jax.nn.silu(gated) * upward).astype(jnp.bfloat16)
        result = jnp.einsum(
            "jrf,jfd->rd", hidden, downs[:, own], preferred_element_type=jnp.float32
        )
        term = result * share
        total = term if total is None else total + term
    weighted = lax.psum_scatter(
        total.astype(jnp.bfloat16), "sp", scatter_dimension=0, tiled=True
    )
    return (stream + weighted.astype(jnp.float32)).astype(jnp.bfloat16)


def solution(mesh):
    return jax.shard_map(
        local,
        mesh=mesh,
        in_specs=(
            P(("grp", "sp"), "tp"),
            P(("grp", "sp"), "tp"),
            P(("grp", "sp"), "tp"),
            P(("grp", "sp"), "tp"),
            P(("grp", "sp"), "tp"),
            P(("grp", "sp"), "tp"),
            P(("grp", "sp"), "tp"),
            P("tp"),
            P("tp"),
            P("tp"),
            P("tp"),
            P("tp", None),
            P(("grp", "sp", "tp"), None),
            P(),
            P(("grp", "sp", "tp"), None),
            P(("grp", "sp", "tp"), None),
            P("sp", None, "tp"),
            P("sp", None, "tp"),
            P("sp", "tp", None),
        ),
        out_specs=P(("grp", "sp", "tp"), None),
        check_vma=False,
    )
```

```python
import functools

import jax
import jax.numpy as jnp
from jax import lax
from jax.experimental import pallas as pl
from jax.experimental.pallas import tpu as pltpu
from jax.sharding import PartitionSpec as P

SPAN = 64
SUB = 16
LANES = 256
GROUP_EPS = 0.00064
NORM_EPS = 1e-06
NN = (((1,), (0,)), ((), ()))
NT = (((1,), (1,)), ((), ()))
TN = (((0,), (0,)), ((), ()))


def halves(x):
    high = x.astype(jnp.bfloat16)
    return high, (x - high.astype(jnp.float32)).astype(jnp.bfloat16)


def product(left, right, dims):
    def dot(a, b):
        return lax.dot_general(a, b, dims, preferred_element_type=jnp.float32)

    return dot(left[0], right[0]) + (dot(left[1], right[0]) + dot(left[0], right[1]))


def block_mask(head_width):
    rows = lax.broadcasted_iota(jnp.int32, (LANES, LANES), 0) // head_width
    lanes = lax.broadcasted_iota(jnp.int32, (LANES, LANES), 1) // head_width
    return jnp.where(rows == lanes, 1.0, 0.0)


def spread_blocks(x, mask):
    copies = LANES // x.shape[0]
    return tuple(jnp.concatenate([part] * copies, axis=0) * mask for part in halves(x))


def head_sum(x, mask):
    high, low = halves(x)
    return lax.dot_general(
        high, mask, NN, preferred_element_type=jnp.float32
    ) + lax.dot_general(low, mask, NN, preferred_element_type=jnp.float32)


def chunk_kernel(
    head_width,
    recept_ref,
    key_ref,
    value_ref,
    decay_ref,
    rate_ref,
    offset_ref,
    decay_bias_ref,
    rate_bias_ref,
    map_ref,
    own_ref,
    transit_ref,
    added_ref,
):
    span = head_width
    wide_mask = block_mask(head_width)
    mask = wide_mask.astype(jnp.bfloat16)
    per_group = LANES // head_width
    times = lax.broadcasted_iota(jnp.int32, (span, LANES), 0)
    lanes = lax.broadcasted_iota(jnp.int32, (span, LANES), 1)
    earlier = lanes % head_width
    strict = times > earlier
    within = times >= earlier
    eye = jnp.where(times == earlier, 1.0, 0.0)
    same = (times // SUB) == (earlier // SUB)
    tri = jnp.where(
        lax.broadcasted_iota(jnp.int32, (span, span), 0)
        >= lax.broadcasted_iota(jnp.int32, (span, span), 1),
        1.0,
        0.0,
    ).astype(jnp.bfloat16)

    @pl.when(pl.program_id(0) == 0)
    def _():
        full_lanes = lax.broadcasted_iota(jnp.int32, transit_ref.shape, 1) % head_width
        full_rows = lax.broadcasted_iota(jnp.int32, transit_ref.shape, 0)
        transit_ref[...] = jnp.where(full_lanes == full_rows, 1.0, 0.0)
        added_ref[...] = jnp.zeros_like(added_ref)

    spread = functools.partial(spread_blocks, mask=mask)
    row_count, channel_width = recept_ref.shape
    cells = [
        (group, chunk)
        for chunk in range(row_count // span)
        for group in range(channel_width // LANES)
    ]

    def prepare(group, chunk):
        at = (slice(chunk * span, (chunk + 1) * span), slice(group * LANES, (group + 1) * LANES))
        cols = at[1]
        recept = recept_ref[at].astype(jnp.float32)
        key = key_ref[at].astype(jnp.float32)
        value = value_ref[at].astype(jnp.float32)
        offset = jnp.zeros((span, LANES), jnp.float32)
        for head in range(per_group):
            column = group * per_group + head
            offset = jnp.where(
                lanes // head_width == head, offset_ref[at[0], column : column + 1], offset
            )
        pre = decay_bias_ref[:, cols] + decay_ref[at].astype(jnp.float32)
        decay = offset - 0.6065306597126334 / (1.0 + jnp.exp(-pre))
        rate = 1.0 / (
            1.0 + jnp.exp(-(rate_bias_ref[:, cols] + rate_ref[at].astype(jnp.float32)))
        )
        unit = key * lax.rsqrt(head_sum(key * key, mask) + NORM_EPS)
        one, rest = halves(decay)
        third = (decay - one.astype(jnp.float32) - rest.astype(jnp.float32)).astype(jnp.bfloat16)
        cumul = sum(
            lax.dot_general(tri, part, NN, preferred_element_type=jnp.float32)
            for part in (third, rest, one)
        )
        middle = cumul[span // 2 : span // 2 + 1]
        last = cumul[span - 1 : span]
        center = cumul - middle
        shrink = jnp.exp(center)
        grow = jnp.exp(-center)
        remove = -unit * jnp.exp(center - decay)
        reads = recept * shrink
        write = unit * rate * grow
        keys = key * grow
        left = halves(jnp.concatenate([remove, reads], axis=0))
        by_write = product(left, spread(write), NT)
        by_key = product(left, spread(keys), NT)
        remove_write = jnp.where(strict, by_write[:span], 0.0)
        read_write = halves(jnp.where(within, by_write[span:], 0.0))
        key_rows = halves(
            jnp.concatenate(
                [jnp.where(strict, by_key[:span], 0.0), jnp.where(within, by_key[span:], 0.0)],
                axis=0,
            )
        )
        power = jnp.where(same, remove_write, 0.0)
        inverse = eye + power
        power = product(halves(power), spread(power), NN)
        reach = 2
        while reach < SUB:
            factor = spread(power)
            if reach * 2 < SUB:
                both = product(
                    halves(jnp.concatenate([inverse, power], axis=0)), factor, NN
                )
                inverse = inverse + both[:span]
                power = both[span:]
            else:
                inverse = inverse + product(halves(inverse), factor, NN)
            reach *= 2
        size = SUB
        while size < span:
            joint = (times // (2 * size) == earlier // (2 * size)) & (
                times // size != earlier // size
            )
            step = product(
                halves(inverse), spread(jnp.where(joint, remove_write, 0.0)), NN
            )
            inverse = inverse + product(halves(step), spread(inverse), NN)
            size *= 2
        inverse = halves(inverse)
        start = jnp.exp(middle)
        from_value = product(key_rows, spread(value), NN)
        inv_remove = product(inverse, spread(remove), NN) * start
        inv_value = product(inverse, spread(from_value[:span]), NN)
        read_map = reads * start + product(read_write, spread(inv_remove), NN)
        read_own = from_value[span:] + product(read_write, spread(inv_value), NN)
        tail = jnp.exp(last - middle)
        write_end = write * tail
        key_end = keys * tail
        transit = product(halves(inv_remove.T), halves(write_end), NN)
        transit = transit * wide_mask
        full = jnp.concatenate([jnp.exp(last)] * (LANES // 8), axis=0)
        full = jnp.concatenate([full] * 8, axis=0)
        diagonal = lax.broadcasted_iota(jnp.int32, (LANES, LANES), 0) == (
            lax.broadcasted_iota(jnp.int32, (LANES, LANES), 1)
        )
        transit = transit + jnp.where(diagonal, full, 0.0)
        added = product(
            halves(jnp.concatenate([inv_value, value], axis=0).T),
            halves(jnp.concatenate([write_end, key_end], axis=0)),
            NN,
        )
        added = added * wide_mask
        added = sum(added[h * head_width : (h + 1) * head_width] for h in range(per_group))
        return at, read_map, read_own, transit, added

    for group, chunk in cells:
        at, read_map, read_own, transit, added = prepare(group, chunk)
        cols = at[1]
        held_transit = transit_ref[:, cols]
        held_added = added_ref[:, cols]
        rows = halves(read_map)
        map_ref[at] = product(rows, spread(held_transit), NT)
        own_ref[at] = read_own + product(rows, spread(held_added), NT)
        moved = product(
            halves(jnp.concatenate([held_transit, held_added], axis=0)), halves(transit), NN
        )
        transit_ref[:, cols] = moved[:span]
        added_ref[:, cols] = moved[span:] + added


def advance_kernel(head_width, state_ref, transit_ref, added_ref, out_ref):
    mask = block_mask(head_width).astype(jnp.bfloat16)
    for group in range(state_ref.shape[1] // LANES):
        cols = slice(group * LANES, (group + 1) * LANES)
        out_ref[:, cols] = added_ref[:, cols] + product(
            halves(state_ref[:, cols]), spread_blocks(transit_ref[:, cols], mask), NN
        )


def finish_kernel(
    head_width,
    map_ref,
    own_ref,
    state_ref,
    recept_ref,
    key_ref,
    value_ref,
    gate_ref,
    gain_ref,
    self_ref,
    out_ref,
):
    mask = block_mask(head_width).astype(jnp.bfloat16)
    for group in range(map_ref.shape[1] // LANES):
        cols = slice(group * LANES, (group + 1) * LANES)
        read = own_ref[:, cols] + product(
            halves(map_ref[:, cols]), spread_blocks(state_ref[:, cols], mask), NT
        )
        off = read - head_sum(read, mask) * (1.0 / head_width)
        spread = head_sum(off * off, mask) * (1.0 / head_width)
        normed = off * lax.rsqrt(spread + GROUP_EPS) * gain_ref[:, cols]
        own = head_sum(
            recept_ref[:, cols].astype(jnp.float32)
            * key_ref[:, cols].astype(jnp.float32)
            * self_ref[:, cols],
            mask,
        ) * value_ref[:, cols].astype(jnp.float32)
        out_ref[:, cols] = ((normed + own) * gate_ref[:, cols].astype(jnp.float32)).astype(
            jnp.bfloat16
        )


def mixer(
    recept,
    key_input,
    value_input,
    output_gate_input,
    decay_input_part,
    correction_rate_input,
    head_decay_offset,
    decay_fixed_bias,
    correction_rate_bias,
    head_norm_gain,
    self_term_weight,
    axis_size,
):
    length, width = recept.shape
    heads = head_decay_offset.shape[1]
    head_width = width // heads
    rows = 2 * SPAN
    by_rows = pl.BlockSpec((rows, width), lambda i: (i, 0))
    fixed = pl.BlockSpec((1, width), lambda i: (0, 0))
    states = pl.BlockSpec((head_width, width), lambda i: (0, 0))
    wide = jax.ShapeDtypeStruct((length, width), jnp.float32)
    small = jax.ShapeDtypeStruct((head_width, width), jnp.float32)
    params = pltpu.CompilerParams(dimension_semantics=("arbitrary",))
    read_map, read_own, transit, added = pl.pallas_call(
        functools.partial(chunk_kernel, head_width),
        grid=(length // rows,),
        in_specs=[by_rows] * 5
        + [pl.BlockSpec((rows, heads), lambda i: (i, 0)), fixed, fixed],
        out_specs=[by_rows, by_rows, states, states],
        out_shape=[wide, wide, small, small],
        compiler_params=params,
        cost_estimate=pl.CostEstimate(
            flops=30_000_000_000, bytes_accessed=8 * length * width, transcendentals=0
        ),
        name="chunks",
    )(
        recept,
        key_input,
        value_input,
        decay_input_part,
        correction_rate_input,
        head_decay_offset,
        decay_fixed_bias[None],
        correction_rate_bias[None],
    )
    place = lax.axis_index("sp")
    state = jnp.zeros_like(added)
    for lap in range(axis_size - 1):
        sent = added
        if lap > 0:
            sent = pl.pallas_call(
                functools.partial(advance_kernel, head_width), out_shape=small, name="advance"
            )(state, transit, added)
        got = lax.ppermute(sent, "sp", [(i, i + 1) for i in range(axis_size - 1)])
        state = jnp.where(place == lap + 1, got, state)
    return pl.pallas_call(
        functools.partial(finish_kernel, head_width),
        grid=(length // rows,),
        in_specs=[by_rows, by_rows, states] + [by_rows] * 4 + [fixed, fixed],
        out_specs=by_rows,
        out_shape=jax.ShapeDtypeStruct((length, width), jnp.bfloat16),
        compiler_params=params,
        cost_estimate=pl.CostEstimate(
            flops=4_000_000_000, bytes_accessed=20 * length * width, transcendentals=0
        ),
        name="finish",
    )(
        read_map,
        read_own,
        state,
        recept,
        key_input,
        value_input,
        output_gate_input,
        head_norm_gain[None],
        self_term_weight[None],
    )


def local(
    recept,
    key_input,
    value_input,
    output_gate_input,
    decay_input_part,
    correction_rate_input,
    head_decay_offset,
    decay_fixed_bias,
    correction_rate_bias,
    head_norm_gain,
    self_term_weight,
    output_weight_matrix,
    residual,
    feedforward_norm_gain,
    routed_expert_index,
    routed_expert_weight,
    gate_weight_experts,
    up_weight_experts,
    down_weight_experts,
):
    gates = lax.all_gather(gate_weight_experts, "tp", axis=0)
    ups = lax.all_gather(up_weight_experts, "tp", axis=0)
    downs = lax.all_gather(down_weight_experts, "tp", axis=0)
    attention_result = mixer(
        recept,
        key_input,
        value_input,
        output_gate_input,
        decay_input_part,
        correction_rate_input,
        head_decay_offset,
        decay_fixed_bias,
        correction_rate_bias,
        head_norm_gain,
        self_term_weight,
        lax.axis_size("sp"),
    )
    part = jnp.dot(
        attention_result, output_weight_matrix, preferred_element_type=jnp.float32
    ).astype(jnp.bfloat16)
    part, gates, ups, downs = lax.optimization_barrier((part, gates, ups, downs))
    proj = lax.psum_scatter(part, "tp", scatter_dimension=0, tiled=True)
    stream = residual.astype(jnp.float32) + lax.optimization_barrier(proj).astype(jnp.float32)
    ffn_in = (
        stream
        * lax.rsqrt(jnp.mean(stream * stream, axis=-1, keepdims=True) + NORM_EPS)
        * feedforward_norm_gain
    ).astype(jnp.bfloat16)
    width = ffn_in.shape[1]
    local_experts = gate_weight_experts.shape[0]
    experts = local_experts * lax.axis_size("sp")
    ids = jnp.arange(experts, dtype=jnp.int32)
    shares = jnp.sum(
        jnp.where(
            routed_expert_index[:, :, None] == ids, routed_expert_weight[:, :, None], 0.0
        ),
        axis=1,
    )
    first = shares.astype(jnp.bfloat16)
    rest = shares - first.astype(jnp.float32)
    second = rest.astype(jnp.bfloat16)
    third = (rest - second.astype(jnp.float32)).astype(jnp.bfloat16)
    extra = jnp.concatenate([first, second, third], axis=1)
    extra = jnp.pad(extra, ((0, 0), (0, -extra.shape[1] % 128)))
    packed = lax.all_gather(
        jnp.concatenate([ffn_in, extra], axis=1), "sp", axis=0, tiled=True
    )
    features = packed[:, :width]
    tail = packed[:, width : width + 3 * experts].astype(jnp.float32)
    shares = tail[:, :experts] + tail[:, experts : 2 * experts] + tail[:, 2 * experts :]
    total = None
    for own in range(local_experts):
        expert = lax.axis_index("sp") * local_experts + own
        share = jnp.sum(jnp.where(ids[None, :] == expert, shares, 0.0), axis=1, keepdims=True)
        gated = jnp.einsum(
            "rd,jdf->jrf", features, gates[:, own], preferred_element_type=jnp.float32
        )
        upward = jnp.einsum(
            "rd,jdf->jrf", features, ups[:, own], preferred_element_type=jnp.float32
        )
        hidden = (jax.nn.silu(gated) * upward).astype(jnp.bfloat16)
        result = jnp.einsum(
            "jrf,jfd->rd", hidden, downs[:, own], preferred_element_type=jnp.float32
        )
        term = result * share
        total = term if total is None else total + term
    weighted = lax.psum_scatter(
        total.astype(jnp.bfloat16), "sp", scatter_dimension=0, tiled=True
    )
    return (stream + weighted.astype(jnp.float32)).astype(jnp.bfloat16)


def solution(mesh):
    return jax.shard_map(
        local,
        mesh=mesh,
        in_specs=(
            P(("grp", "sp"), "tp"),
            P(("grp", "sp"), "tp"),
            P(("grp", "sp"), "tp"),
            P(("grp", "sp"), "tp"),
            P(("grp", "sp"), "tp"),
            P(("grp", "sp"), "tp"),
            P(("grp", "sp"), "tp"),
            P("tp"),
            P("tp"),
            P("tp"),
            P("tp"),
            P("tp", None),
            P(("grp", "sp", "tp"), None),
            P(),
            P(("grp", "sp", "tp"), None),
            P(("grp", "sp", "tp"), None),
            P("sp", None, "tp"),
            P("sp", None, "tp"),
            P("sp", "tp", None),
        ),
        out_specs=P(("grp", "sp", "tp"), None),
        check_vma=False,
    )
```
